32 devices in a mesh: sp: 8 (over z, y), tp: 4 (over x, core).
Axes of the slice: x: 2, y: 2, z: 4, core: 2. Of those that a mesh axis runs over, the one named last changes fastest.
Arguments:
- queries: bfloat16 [8192, 1024], P('sp', 'tp'), may hold values from -6 to 6
- keys: bfloat16 [8192, 1024], P('sp', 'tp'), may hold values from -6 to 6
- values: bfloat16 [8192, 2048], P('sp', 'tp'), may hold values from -6 to 6
- output_gate_logits: bfloat16 [8192, 2048], P('sp', 'tp'), may hold values from -6 to 6
- log_input_gate: float32 [16, 8192], P('tp', 'sp'), may hold values from -4 to 104, as said below
- forget_gate_logits: float32 [16, 8192], P('tp', 'sp'), may hold values from 1 to 20
- extra_forget_terms: float32 [16, 8192], P('tp', 'sp'), may hold values from -2.1 to 0, as said below
- per_head_norm_gain: float32 [2048], P('tp'), may hold values from 0.1 to 1.9
- output_weight: bfloat16 [2048, 2048], P('tp'), may hold values from -0.125 to 0.125
- residual: bfloat16 [8192, 2048], P(('sp', 'tp')), may hold values from -6 to 6
- after_cell_norm_gain: float32 [2048], replicated, may hold values from 0.1 to 1.9
- feedforward_norm_gain: float32 [2048], replicated, may hold values from 0.1 to 1.9
- closing_norm_gain: float32 [2048], replicated, may hold values from 0.1 to 1.9
- gate_up_weight: bfloat16 [2048, 5632], P('sp', 'tp'), may hold values from -0.125 to 0.125
- value_up_weight: bfloat16 [2048, 5632], P('sp', 'tp'), may hold values from -0.125 to 0.125
- gate_filter_taps: bfloat16 [3, 5632], P(None, 'tp'), may hold values from -3 to 3
- value_filter_taps: bfloat16 [3, 5632], P(None, 'tp'), may hold values from -3 to 3
- down_weight: bfloat16 [5632, 2048], P('tp', 'sp'), may hold values from -0.078125 to 0.078125
Outputs:
- result: bfloat16 [8192, 2048], P(('sp', 'tp'))
The draws below stay inside these ranges and needn't reach their ends.
Inputs may be any that keep to these rules, and one draw needn't show every extreme that they name: log_input_gate is a log gate of order one at most positions and may be far larger at a few. extra_forget_terms is zero at nearly all positions.
All inputs are finite; a program needn't handle non-finite values.
Results may differ from the reference program's by a relative error of at most 0.019.
Values may be sent and summed in bfloat16 or wider, within the bound.
A program may use at most 128 MiB of HBM per device.

```python
import jax
import jax.numpy as jnp
from jax import lax

D = 2048
HEADS = 16
KEY_DIM = 64
VAL_DIM = 128
FF = 5632
WIDTH = 3
BLOCK = 64
TOK_DEV = 1024
TOKENS = 8192
N_TP = 4


def draw_log_input_gate(key, part):
    first = jax.random.fold_in(key, 0)
    return jax.random.truncated_normal(first, -4.0, 4.0, (HEADS, TOKENS), jnp.float32)


def draw_forget_gate_logits(key, part):
    parts_keys = jax.random.split(key, 5)
    share = 0.5
    slow = jax.random.uniform(parts_keys[0], (HEADS, 1), jnp.float32) < share
    slow_rate = jax.random.uniform(parts_keys[1], (HEADS, 1), jnp.float32, 0.2, 0.8) / TOKENS
    fast_rate = jax.random.uniform(parts_keys[2], (HEADS, 1), jnp.float32, 0.01, 0.033)
    blocks = TOKENS // TOK_DEV
    factor = jnp.exp(jax.random.uniform(parts_keys[3], (1, blocks), jnp.float32, -0.7, 0.7))
    factor = jnp.repeat(factor, TOK_DEV, axis=1)
    noise = jnp.exp(0.5 * jax.random.truncated_normal(parts_keys[4], -2.0, 2.0, (HEADS, TOKENS), jnp.float32))
    rate = jnp.where(slow, slow_rate, fast_rate) * factor * noise
    return -jnp.log(jnp.expm1(rate))


def draw_extra_forget_terms(key, part):
    first, second = jax.random.split(key, 2)
    spots = jax.random.randint(first, (HEADS, 3), 0, TOKENS)
    drops = -jax.random.uniform(second, (HEADS, 3), jnp.float32, 0.22, 0.69)
    places = jnp.arange(TOKENS)[None, None, :] == spots[:, :, None]
    return jnp.sum(jnp.where(places, drops[:, :, None], 0.0), axis=1)


def shard_levels(key, extent, pieces, smallest, top_value):
    factor_of = 1.0
    for position, parts in pieces:
        steps = jax.random.uniform(jax.random.fold_in(jax.random.fold_in(key, 6), position), (parts,), jnp.float32, smallest / len(pieces), top_value / len(pieces))
        factor_of = factor_of * jnp.repeat(jnp.exp(steps), extent[position] // parts).reshape((-1,) + (1,) * (len(extent) - 1 - position))
    return factor_of


def gaussian(own_key, dims, width, reach, shards=(), kind=jnp.bfloat16):
    factor_of = shard_levels(own_key, dims, shards, -0.22, 0.18) if shards else 1.0
    drawn = jax.random.normal(own_key, dims, jnp.float32) * width * factor_of
    return jnp.minimum(jnp.maximum(drawn, -reach), reach).astype(kind)


def setup_inputs(seed: int = 0) -> dict:
    seeds = jax.random.split(jax.random.key(seed), 19)
    return {
        "queries": gaussian(seeds[0], (TOKENS, HEADS * KEY_DIM), 1.0, 6.0, ((0, 8), (1, 4))),
        "keys": gaussian(seeds[1], (TOKENS, HEADS * KEY_DIM), 1.0, 6.0, ((0, 8), (1, 4))),
        "values": gaussian(seeds[2], (TOKENS, HEADS * VAL_DIM), 1.0, 6.0, ((0, 8), (1, 4))),
        "output_gate_logits": gaussian(seeds[3], (TOKENS, HEADS * VAL_DIM), 1.0, 6.0, ((0, 8), (1, 4))),
        "log_input_gate": draw_log_input_gate(jax.random.fold_in(seeds[18], 71), 0),
        "forget_gate_logits": draw_forget_gate_logits(jax.random.fold_in(seeds[18], 71), 0),
        "extra_forget_terms": draw_extra_forget_terms(jax.random.fold_in(seeds[18], 71), 0),
        "per_head_norm_gain": jnp.clip(1.0 + 0.18 * jax.random.normal(seeds[7], (HEADS * VAL_DIM,), jnp.float32), 0.1, 1.9),
        "output_weight": gaussian(seeds[8], (HEADS * VAL_DIM, D), (HEADS * VAL_DIM) ** -0.5, 0.125, ((0, 4),)),
        "residual": gaussian(seeds[9], (TOKENS, D), 1.0, 6.0, ((0, 32),)),
        "after_cell_norm_gain": jnp.clip(1.0 + 0.18 * jax.random.normal(seeds[10], (D,), jnp.float32), 0.1, 1.9),
        "feedforward_norm_gain": jnp.clip(1.0 + 0.18 * jax.random.normal(seeds[11], (D,), jnp.float32), 0.1, 1.9),
        "closing_norm_gain": jnp.clip(1.0 + 0.18 * jax.random.normal(seeds[12], (D,), jnp.float32), 0.1, 1.9),
        "gate_up_weight": gaussian(seeds[13], (D, FF), D ** -0.5, 0.125, ((0, 8), (1, 4))),
        "value_up_weight": gaussian(seeds[14], (D, FF), D ** -0.5, 0.125, ((0, 8), (1, 4))),
        "gate_filter_taps": gaussian(seeds[15], (WIDTH, FF), 0.577, 3.0, ((1, 4),)),
        "value_filter_taps": gaussian(seeds[16], (WIDTH, FF), 0.577, 3.0, ((1, 4),)),
        "down_weight": gaussian(seeds[17], (FF, D), FF ** -0.5, 0.078125, ((0, 4), (1, 8))),
    }


eps = 1e-06
exact_mode = lax.Precision.HIGHEST

def block_step(carried_in, inputs):
    state_cells, state_norm, state_max = carried_in
    queries_blk, keys_blk, values_blk, gate_in, gate_log = inputs
    span_len = queries_blk.shape[1]
    causal = jnp.tril(jnp.ones((span_len, span_len), dtype=bool))
    cum_log = jnp.cumsum(gate_log, axis=-1)
    decay_log = jnp.where(causal, cum_log[:, :, None] - cum_log[:, None, :] + gate_in[:, None, :], -jnp.inf)
    carried_log = cum_log + state_max[:, None]
    top_log = jnp.maximum(carried_log, lax.optimization_barrier(jnp.max(decay_log, axis=-1)))
    scores = jnp.einsum('htd,hsd->hts', queries_blk, keys_blk, precision=exact_mode) * jnp.exp(decay_log - top_log[:, :, None])
    carried_weight = jnp.exp(carried_log - top_log)
    numerator = jnp.einsum('hts,hse->hte', scores, values_blk, precision=exact_mode)
    numerator = numerator + carried_weight[:, :, None] * jnp.einsum('htd,hde->hte', queries_blk, state_cells, precision=exact_mode)
    denominator = lax.optimization_barrier(jnp.sum(scores, axis=-1)) + carried_weight * jnp.einsum('htd,hd->ht', queries_blk, state_norm, precision=exact_mode)
    output = numerator / jnp.maximum(jnp.abs(denominator), jnp.exp(-top_log))[:, :, None]
    last_log = cum_log[:, -1]
    gain_log = last_log[:, None] - cum_log + gate_in
    next_max = jnp.maximum(last_log + state_max, lax.optimization_barrier(jnp.max(gain_log, axis=-1)))
    fade_out = jnp.exp(last_log + state_max - next_max)
    weighted = jnp.exp(gain_log - next_max[:, None])[:, :, None] * keys_blk
    next_cells = fade_out[:, None, None] * state_cells + jnp.einsum('hsd,hse->hde', weighted, values_blk, precision=exact_mode)
    next_norm = fade_out[:, None] * state_norm + lax.optimization_barrier(jnp.sum(weighted, axis=1))
    return ((next_cells, next_norm, next_max), output)

def split_heads(array, head_count, head_width, blocks):
    return array.astype(jnp.float32).reshape(blocks, BLOCK, head_count, head_width).transpose(0, 2, 1, 3)

def gate_blocks(array, blocks):
    return array.reshape(array.shape[0], blocks, BLOCK).transpose(1, 0, 2)

def rms_gain(inputs, gains):
    return inputs * lax.rsqrt(lax.optimization_barrier(jnp.mean(inputs * inputs, axis=-1, keepdims=True)) + eps) * gains

def split_sum(left_side, right_side, shard_count):
    shard_width = left_side.shape[1] // shard_count
    running = jnp.zeros((left_side.shape[0], right_side.shape[1]), jnp.float32)
    for shard_idx in range(shard_count):
        lower = shard_idx * shard_width
        part_sum = jnp.dot(left_side[:, lower:lower + shard_width], right_side[lower:lower + shard_width], preferred_element_type=jnp.float32)
        rounded = lax.optimization_barrier(part_sum.astype(jnp.bfloat16))
        running = running + rounded.astype(jnp.float32)
    return running

def causal_conv(rows_in, kernel_taps):
    length = rows_in.shape[0]
    padded = jnp.pad(rows_in.astype(jnp.float32), ((WIDTH - 1, 0), (0, 0)))
    summed = jnp.zeros(rows_in.shape, jnp.float32)
    for offset in range(WIDTH):
        summed = summed + kernel_taps[offset].astype(jnp.float32) * padded[offset:offset + length]
    return summed

def reference(queries, keys, values, output_gate_logits, log_input_gate, forget_gate_logits, extra_forget_terms, per_head_norm_gain, output_weight, residual, after_cell_norm_gain, feedforward_norm_gain, closing_norm_gain, gate_up_weight, value_up_weight, gate_filter_taps, value_filter_taps, down_weight):
    blocks = TOKENS // BLOCK
    query_scale = KEY_DIM ** (-0.5)
    queries_f = split_heads(queries, HEADS, KEY_DIM, blocks) * query_scale
    keys_f = split_heads(keys, HEADS, KEY_DIM, blocks)
    values_f = split_heads(values, HEADS, VAL_DIM, blocks)
    log_forget_terms = jax.nn.log_sigmoid(forget_gate_logits) + extra_forget_terms
    start = (jnp.zeros((HEADS, KEY_DIM, VAL_DIM), jnp.float32), jnp.zeros((HEADS, KEY_DIM), jnp.float32), jnp.zeros((HEADS,), jnp.float32))
    _, cell_out = lax.scan(block_step, start, (queries_f, keys_f, values_f, gate_blocks(log_input_gate, blocks), gate_blocks(log_forget_terms, blocks)))
    cell_out = cell_out.transpose(0, 2, 1, 3).reshape(TOKENS, HEADS * VAL_DIM)
    mixed = cell_out * per_head_norm_gain * jax.nn.sigmoid(output_gate_logits.astype(jnp.float32))
    mixed = mixed.astype(jnp.bfloat16)
    mixer_out = split_sum(mixed, output_weight, N_TP).astype(jnp.bfloat16)
    after_mixer = (residual.astype(jnp.float32) + rms_gain(mixer_out.astype(jnp.float32), after_cell_norm_gain)).astype(jnp.bfloat16)
    normed = rms_gain(after_mixer.astype(jnp.float32), feedforward_norm_gain).astype(jnp.bfloat16)
    gate_rows = jnp.dot(normed, gate_up_weight, preferred_element_type=jnp.float32).astype(jnp.bfloat16)
    value_rows = jnp.dot(normed, value_up_weight, preferred_element_type=jnp.float32).astype(jnp.bfloat16)
    gate_conv = causal_conv(gate_rows, gate_filter_taps)
    value_conv = causal_conv(value_rows, value_filter_taps)
    activated = (jax.nn.gelu(gate_conv, approximate=True) * value_conv).astype(jnp.bfloat16)
    ffn_out = split_sum(activated, down_weight, N_TP).astype(jnp.bfloat16)
    return (after_mixer.astype(jnp.float32) + rms_gain(ffn_out.astype(jnp.float32), closing_norm_gain)).astype(jnp.bfloat16)
```

```python
import functools

import jax
import jax.numpy as jnp
from jax import lax
from jax.experimental import pallas as pl
from jax.experimental.pallas import tpu as pltpu
from jax.sharding import PartitionSpec as P

MESH = pl.DeviceIdType.MESH
CORES = 2
VMEM_LIMIT = 60 * 1024 * 1024

KEY_DIM = 64
VAL_DIM = 128
WIDTH = 3
BLOCK = 64


eps = 1e-06
empty_log = -1e30
exact_mode = lax.Precision.HIGHEST


def entering(cells, norm, top, total):
    heads, width, depth = cells.shape
    spare = jnp.zeros((heads, 8, depth), jnp.float32)
    spare = spare.at[:, 0, :width].set(norm)
    spare = spare.at[:, 1, :].set(top[:, None]).at[:, 2, :].set(total[:, None])
    pieces = gather_states(jnp.concatenate([cells, spare], axis=1))
    count, mine = lax.axis_size("sp"), lax.axis_index("sp")
    tops, totals = pieces[:, :, width + 1, 0], pieces[:, :, width + 2, 0]
    place = jnp.arange(count)[:, None]
    before = place < mine
    held = jnp.where(before, totals, 0.0)
    after = jnp.sum(held, axis=0) - jnp.cumsum(held, axis=0)
    reach = jnp.where(before, after + tops, empty_log)
    best = jnp.max(reach, axis=0)
    factor = jnp.where(before, jnp.exp(reach - best), 0.0)
    merged = jnp.sum(factor[:, :, None, None] * pieces[:, :, : width + 1, :], axis=0)
    return merged[:, :width], merged[:, width, :width], best


def passed_along(array, axis, by):
    count = lax.axis_size(axis)
    pairs = [(i, i + by) for i in range(count) if 0 <= i + by < count]
    return lax.ppermute(array, axis, pairs)


def cell_blocks(queries, keys, values, gate_in, log_forget_terms, in_cells, in_norm, in_max):
    tok_rows = queries.shape[0]
    head_count = gate_in.shape[0]
    blocks = tok_rows // BLOCK
    scale = KEY_DIM ** (-0.5)
    query_bf = queries.reshape(blocks, BLOCK, head_count, KEY_DIM)
    key_bf = keys.reshape(blocks, BLOCK, head_count, KEY_DIM)
    value_f = values.astype(jnp.float32).reshape(blocks, BLOCK, head_count, VAL_DIM)
    query_f = query_bf.astype(jnp.float32) * scale
    gate_blk = gate_in.reshape(head_count, blocks, BLOCK).transpose(1, 0, 2)
    log_blk = log_forget_terms.reshape(head_count, blocks, BLOCK).transpose(1, 0, 2)
    cum_log = jnp.cumsum(log_blk, axis=-1)
    last_log = cum_log[..., -1]
    gain_log = last_log[..., None] - cum_log + gate_blk
    block_max = jnp.max(gain_log, axis=-1)
    fades = jnp.exp(gain_log - block_max[..., None]).transpose(0, 2, 1)
    weighted_keys = fades[..., None] * key_bf.astype(jnp.float32)
    block_cells = jnp.einsum("bshd,bshe->bhde", weighted_keys, value_f, precision=exact_mode)
    block_norm = jnp.sum(weighted_keys, axis=1)
    inclusive = jnp.cumsum(last_log, axis=0)
    exclusive = inclusive - last_log
    lower = (jnp.arange(blocks)[:, None] > jnp.arange(blocks)[None, :])[:, :, None]
    reach_log = jnp.where(
        lower, exclusive[:, None, :] - inclusive[None, :, :] + block_max[None], empty_log
    )
    device_log = exclusive + in_max[None, :]
    top_in = jnp.maximum(jnp.max(reach_log, axis=1), device_log)
    factor = jnp.where(lower, jnp.exp(reach_log - top_in[:, None, :]), 0.0)
    device_factor = jnp.exp(device_log - top_in)
    cells_in = (
        jnp.einsum("bjh,jhde->bhde", factor, block_cells, precision=exact_mode)
        + device_factor[..., None, None] * in_cells[None]
    )
    norm_in = (
        jnp.einsum("bjh,jhd->bhd", factor, block_norm, precision=exact_mode)
        + device_factor[..., None] * in_norm[None]
    )
    causal = jnp.tril(jnp.ones((BLOCK, BLOCK), dtype=bool))
    decay_log = jnp.where(
        causal, cum_log[..., :, None] - cum_log[..., None, :] + gate_blk[..., None, :], -jnp.inf
    )
    carried_log = cum_log + top_in[..., None]
    top_log = jnp.maximum(carried_log, jnp.max(decay_log, axis=-1))
    products = (
        jnp.einsum("bthd,bshd->bhts", query_bf, key_bf, preferred_element_type=jnp.float32) * scale
    )
    scores = products * jnp.exp(decay_log - top_log[..., None])
    carried_weight = jnp.exp(carried_log - top_log)
    numerator = jnp.einsum("bhts,bshe->bhte", scores, value_f, precision=exact_mode)
    numerator = numerator + carried_weight[..., None] * jnp.einsum(
        "bthd,bhde->bhte", query_f, cells_in, precision=exact_mode
    )
    denominator = jnp.sum(scores, axis=-1) + carried_weight * jnp.einsum(
        "bthd,bhd->bht", query_f, norm_in, precision=exact_mode
    )
    output = numerator / jnp.maximum(jnp.abs(denominator), jnp.exp(-top_log))[..., None]
    return output.transpose(0, 2, 1, 3).reshape(tok_rows, head_count * VAL_DIM)


def rms_gain(inputs, gains):
    return inputs * lax.rsqrt(jnp.mean(inputs * inputs, axis=-1, keepdims=True) + eps) * gains


def remote(src, dst, send, recv, where):
    return pltpu.make_async_remote_copy(
        src_ref=src,
        dst_ref=dst,
        send_sem=send,
        recv_sem=recv,
        device_id=where,
        device_id_type=MESH,
    )


def greet(targets):
    barrier = pltpu.get_barrier_semaphore()
    for where in targets:
        pl.semaphore_signal(barrier, inc=1, device_id=where, device_id_type=MESH)
    pl.semaphore_wait(barrier, len(targets))


def state_kernel(rows_z, rows_y, mine_ref, all_ref, z_send, z_recv, y_send, y_recv):
    me = lax.axis_index("sp")
    at_z, at_y = me // rows_y, lax.rem(me, rows_y)
    column = [lax.rem(at_z + k, rows_z) * rows_y + at_y for k in range(rows_z)]
    behind = [lax.rem(at_z + rows_z - k, rows_z) * rows_y + at_y for k in range(rows_z)]
    ahead_y = [lax.rem(at_y + k, rows_y) for k in range(rows_y)]
    behind_y = [lax.rem(at_y + rows_y - k, rows_y) for k in range(rows_y)]
    greet(
        [{"sp": column[k]} for k in range(1, rows_z)]
        + [{"sp": at_z * rows_y + ahead_y[k]} for k in range(1, rows_y)]
    )
    all_ref[me] = mine_ref[...]
    copies = []
    for k in range(1, rows_z):
        copies.append(
            remote(mine_ref, all_ref.at[me], z_send.at[k], z_recv.at[k], {"sp": column[k]})
        )
        copies[-1].start()
    arriving = []
    for d in range(rows_z):
        source = behind[d]
        if d:
            remote(
                mine_ref, all_ref.at[source], z_send.at[d], z_recv.at[d], {"sp": source}
            ).wait_recv()
        for k in range(1, rows_y):
            where = {"sp": at_z * rows_y + ahead_y[k]}
            block = mine_ref if d == 0 else all_ref.at[source]
            copies.append(
                remote(block, all_ref.at[source], y_send.at[d, k], y_recv.at[d, k], where)
            )
            copies[-1].start()
            from_block = all_ref.at[source - at_y + behind_y[k]]
            arriving.append(
                remote(mine_ref, from_block, y_send.at[d, k], y_recv.at[d, k], where)
            )
    for copy in arriving:
        copy.wait_recv()
    for copy in copies:
        copy.wait_send()


def gather_states(packed):
    count = lax.axis_size("sp")
    rows_y = 1
    while 8 * rows_y * rows_y <= count:
        rows_y *= 2
    rows_z = count // rows_y
    dma = pltpu.SemaphoreType.DMA
    return pl.pallas_call(
        functools.partial(state_kernel, rows_z, rows_y),
        out_shape=jax.ShapeDtypeStruct((count,) + packed.shape, packed.dtype),
        in_specs=[pl.BlockSpec(memory_space=pltpu.VMEM)],
        out_specs=pl.BlockSpec(memory_space=pltpu.VMEM),
        scratch_shapes=[
            dma((rows_z,)),
            dma((rows_z,)),
            dma((rows_z, rows_y)),
            dma((rows_z, rows_y)),
        ],
        compiler_params=pltpu.CompilerParams(
            collective_id=0, has_side_effects=True, vmem_limit_bytes=32 * 1024 * 1024
        ),
        cost_estimate=pl.CostEstimate(flops=10**8, bytes_accessed=10**6, transcendentals=0),
        name="states",
    )(packed)


def reduce_rows(
    count, pieces, left_ref, right_ref, total, pair_out, pair_in, x_out, x_in, sems, partner, peers
):
    pair_send, pair_recv, x_send, x_recv = sems
    me = lax.axis_index("tp")
    at_x, core = me // CORES, lax.rem(me, CORES)
    rows = left_ref.shape[0] // count
    xs = count // CORES
    step = rows // pieces
    width = right_ref.shape[1]
    tile = 512 if width % 512 == 0 else width

    def product(chunk, piece, store):
        start = pl.multiple_of(chunk * rows + piece * step, step)
        left = left_ref[pl.ds(start, step), :]

        @pl.loop(0, width // tile)
        def _(j):
            cols = pl.ds(pl.multiple_of(j * tile, tile), tile)
            store(cols, jnp.dot(left, right_ref[:, cols], preferred_element_type=jnp.float32))

    sent, landing = [], []
    for k in list(range(1, xs)) + [0]:
        to_x = lax.rem(at_x + k, xs)
        for s in range(pieces):
            span = pl.ds(s * step, step)

            def put_pair(cols, block, k=k, span=span):
                pair_out[k, span, cols] = block.astype(jnp.bfloat16)

            product(to_x * CORES + 1 - core, s, put_pair)
            copy = remote(
                pair_out.at[k, span],
                pair_in.at[k, span],
                pair_send.at[k, s],
                pair_recv.at[k, s],
                {"tp": partner},
            )
            copy.start()
            sent.append(copy)

            def put_own(cols, block, span=span):
                total[span, cols] = block.astype(jnp.bfloat16).astype(jnp.float32)

            product(to_x * CORES + core, s, put_own)
            copy.wait_recv()
            summed = total[span, :] + pair_in[k, span, :].astype(jnp.float32)
            if k == 0:
                total[span, :] = summed
            else:
                x_out[k - 1, span, :] = summed.astype(jnp.bfloat16)
                copy = remote(
                    x_out.at[k - 1, span],
                    x_in.at[k - 1, span],
                    x_send.at[k, s],
                    x_recv.at[k, s],
                    {"tp": peers[k]},
                )
                copy.start()
                sent.append(copy)
                landing.append((s, copy))
    return landing, sent


def tp_places(count):
    me = lax.axis_index("tp")
    at_x, core = me // CORES, lax.rem(me, CORES)
    xs = count // CORES
    partner = at_x * CORES + 1 - core
    peers = [lax.rem(at_x + k, xs) * CORES + core for k in range(xs)]
    sources = [lax.rem(at_x + xs - k, xs) * CORES + core for k in range(xs)]
    return me, partner, peers, sources


def finish_piece(count, s, landing, total, x_in, step):
    span = pl.ds(s * step, step)
    for at, copy in landing:
        if at == s:
            copy.wait_recv()
    summed = total[span, :]
    for k in range(1, count // CORES):
        summed = summed + x_in[k - 1, span, :].astype(jnp.float32)
    return span, summed.astype(jnp.bfloat16).astype(jnp.float32)


def mixer_kernel(
    count, pieces, mixed_ref, weight_ref, residual_ref, gain_ref, next_gain_ref,
    after_ref, normed_ref,
    total, pair_out, pair_in, x_out, x_in,
    pair_send, pair_recv, x_send, x_recv, gx_send, gx_recv, gp_send, gp_recv,
):
    me, partner, peers, sources = tp_places(count)
    xs = count // CORES
    rows = mixed_ref.shape[0] // count
    step = rows // pieces
    greet([{"tp": partner}] + [{"tp": peers[k]} for k in range(1, xs)])
    landing, sent = reduce_rows(
        count, pieces, mixed_ref, weight_ref, total, pair_out, pair_in, x_out, x_in,
        (pair_send, pair_recv, x_send, x_recv), partner, peers,
    )

    def block(device, s):
        return normed_ref.at[pl.ds(pl.multiple_of(device * rows + s * step, step), step)]

    for s in range(pieces):
        span, mixer_out = finish_piece(count, s, landing, total, x_in, step)
        after = residual_ref[span, :].astype(jnp.float32) + rms_gain(mixer_out, gain_ref[...])
        after = after.astype(jnp.bfloat16)
        after_ref[span, :] = after
        normed = rms_gain(after.astype(jnp.float32), next_gain_ref[...])
        normed_ref[pl.ds(pl.multiple_of(me * rows + s * step, step), step), :] = normed.astype(
            jnp.bfloat16
        )
        own = block(me, s)
        for k in range(1, xs):
            sent.append(remote(own, own, gx_send.at[k, s], gx_recv.at[k, s], {"tp": peers[k]}))
            sent[-1].start()
        sent.append(remote(own, own, gp_send.at[0, s], gp_recv.at[0, s], {"tp": partner}))
        sent[-1].start()
    for s in range(pieces):
        for k in range(1, xs):
            came = block(sources[k], s)
            remote(came, came, gx_send.at[k, s], gx_recv.at[k, s], {"tp": peers[k]}).wait_recv()
            sent.append(remote(came, came, gp_send.at[k, s], gp_recv.at[k, s], {"tp": partner}))
            sent[-1].start()
    for s in range(pieces):
        for k in range(xs):
            came = block(sources[k] + partner - me, s)
            remote(came, came, gp_send.at[k, s], gp_recv.at[k, s], {"tp": partner}).wait_recv()
    for copy in sent:
        copy.wait_send()


def closing_kernel(
    count, pieces, active_ref, weight_ref, after_ref, gain_ref,
    out_ref,
    total, pair_out, pair_in, x_out, x_in,
    pair_send, pair_recv, x_send, x_recv,
):
    me, partner, peers, sources = tp_places(count)
    xs = count // CORES
    rows = active_ref.shape[0] // count
    step = rows // pieces
    greet([{"tp": partner}] + [{"tp": peers[k]} for k in range(1, xs)])
    landing, sent = reduce_rows(
        count, pieces, active_ref, weight_ref, total, pair_out, pair_in, x_out, x_in,
        (pair_send, pair_recv, x_send, x_recv), partner, peers,
    )
    for s in range(pieces):
        span, ffn_out = finish_piece(count, s, landing, total, x_in, step)
        result = after_ref[span, :].astype(jnp.float32) + rms_gain(ffn_out, gain_ref[...])
        out_ref[span, :] = result.astype(jnp.bfloat16)
    for copy in sent:
        copy.wait_send()


def fused_rows(kernel, name, number, pieces, outs, gathers, left, right, *others):
    count = lax.axis_size("tp")
    xs = count // CORES
    rows, width = left.shape[0] // count, right.shape[1]
    dma = pltpu.SemaphoreType.DMA((xs, pieces))
    vmem = pl.BlockSpec(memory_space=pltpu.VMEM)
    return pl.pallas_call(
        functools.partial(kernel, count, pieces),
        out_shape=outs,
        in_specs=[vmem] * (2 + len(others)),
        out_specs=jax.tree.map(lambda _: vmem, outs),
        scratch_shapes=[
            pltpu.VMEM((rows, width), jnp.float32),
            pltpu.VMEM((xs, rows, width), jnp.bfloat16),
            pltpu.VMEM((xs, rows, width), jnp.bfloat16),
            pltpu.VMEM((max(xs - 1, 1), rows, width), jnp.bfloat16),
            pltpu.VMEM((max(xs - 1, 1), rows, width), jnp.bfloat16),
        ]
        + [dma] * (8 if gathers else 4),
        compiler_params=pltpu.CompilerParams(
            collective_id=number, has_side_effects=True, vmem_limit_bytes=48 * 1024 * 1024
        ),
        cost_estimate=pl.CostEstimate(
            flops=2 * left.shape[0] * left.shape[1] * width,
            bytes_accessed=10**7,
            transcendentals=0,
        ),
        name=name,
    )(left, right, *others)


def causal_conv(padded, kernel_taps):
    length = padded.shape[0] - WIDTH + 1
    summed = jnp.zeros((length, padded.shape[1]), jnp.float32)
    for offset in range(WIDTH):
        summed = summed + kernel_taps[offset].astype(jnp.float32) * padded[
            offset : offset + length
        ].astype(jnp.float32)
    return summed


def shards(
    queries,
    keys,
    values,
    output_gate_logits,
    log_input_gate,
    forget_gate_logits,
    extra_forget_terms,
    per_head_norm_gain,
    output_weight,
    residual,
    after_cell_norm_gain,
    feedforward_norm_gain,
    closing_norm_gain,
    gate_up_weight,
    value_up_weight,
    gate_filter_taps,
    value_filter_taps,
    down_weight,
):
    tok_rows = queries.shape[0]
    head_count = log_input_gate.shape[0]
    hidden_cols = gate_up_weight.shape[1]
    up_full, down_full = (
        lax.all_gather(
            jnp.concatenate([gate_up_weight, value_up_weight], axis=1), "sp", axis=0, tiled=True
        ),
        lax.all_gather(down_weight, "sp", axis=1, tiled=True),
    )
    log_forget_terms = jax.nn.log_sigmoid(forget_gate_logits) + extra_forget_terms
    cum_forget = jnp.cumsum(log_forget_terms, axis=1)
    total_log = cum_forget[:, -1]
    flat_keys = keys.astype(jnp.float32).reshape(tok_rows, head_count, KEY_DIM).transpose(1, 0, 2)
    flat_values = (
        values.astype(jnp.float32).reshape(tok_rows, head_count, VAL_DIM).transpose(1, 0, 2)
    )
    reach_log = total_log[:, None] - cum_forget + log_input_gate
    local_max = jnp.max(reach_log, axis=1)
    weighted = jnp.exp(reach_log - local_max[:, None])[:, :, None] * flat_keys
    local_cells = jnp.einsum("hsd,hse->hde", weighted, flat_values, precision=exact_mode)
    local_norm = jnp.sum(weighted, axis=1)
    in_cells, in_norm, in_max = entering(local_cells, local_norm, local_max, total_log)
    cell_out = cell_blocks(
        queries, keys, values, log_input_gate, log_forget_terms, in_cells, in_norm, in_max
    )
    mixed = cell_out * per_head_norm_gain * jax.nn.sigmoid(output_gate_logits.astype(jnp.float32))
    mixed = mixed.astype(jnp.bfloat16)
    width = output_weight.shape[1]
    own_rows = jax.ShapeDtypeStruct(residual.shape, jnp.bfloat16)
    all_rows = jax.ShapeDtypeStruct((tok_rows, width), jnp.bfloat16)
    after_mixer, normed = fused_rows(
        mixer_kernel, "mixer", 1, 2, (own_rows, all_rows), True,
        mixed, output_weight, residual,
        after_cell_norm_gain.reshape(1, -1), feedforward_norm_gain.reshape(1, -1),
    )
    lifted = jnp.dot(normed, up_full, preferred_element_type=jnp.float32)
    gate_sum = lifted[:, :hidden_cols]
    value_sum = lifted[:, hidden_cols:]
    gate_rows = gate_sum.astype(jnp.bfloat16)
    value_rows = value_sum.astype(jnp.bfloat16)
    tail_from = tok_rows - WIDTH + 1
    prior_gate, prior_value = passed_along((gate_rows[tail_from:], value_rows[tail_from:]), "sp", 1)
    gate_conv = causal_conv(jnp.concatenate([prior_gate, gate_rows], axis=0), gate_filter_taps)
    value_conv = causal_conv(jnp.concatenate([prior_value, value_rows], axis=0), value_filter_taps)
    activated = (jax.nn.gelu(gate_conv, approximate=True) * value_conv).astype(jnp.bfloat16)
    return fused_rows(
        closing_kernel, "closing", 2, 2, own_rows, False,
        activated, down_full, after_mixer, closing_norm_gain.reshape(1, -1),
    )


def solution(mesh):
    placed = (
        P("sp", "tp"),
        P("sp", "tp"),
        P("sp", "tp"),
        P("sp", "tp"),
        P("tp", "sp"),
        P("tp", "sp"),
        P("tp", "sp"),
        P("tp"),
        P("tp", None),
        P(("sp", "tp"), None),
        P(),
        P(),
        P(),
        P("sp", "tp"),
        P("sp", "tp"),
        P(None, "tp"),
        P(None, "tp"),
        P("tp", "sp"),
    )
    return jax.shard_map(
        shards, mesh=mesh, in_specs=placed, out_specs=P(("sp", "tp"), None), check_vma=False
    )
```
